32 devices in a mesh: sp: 8 (over z, x), tp: 4 (over y, core).
Axes of the slice: x: 2, y: 2, z: 4, core: 2. Of those that a mesh axis runs over, the one named last changes fastest.
Arguments:
- mixer_out: bfloat16 [1024, 2048], P('sp'), may hold values from -6 to 6
- out_grad: bfloat16 [1024, 2048], P('sp'), may hold values from -2 to 2
- route_ids: int32 [1024, 2], P('sp'), may hold values from 0 to 7, all different within a row; in each aligned block of 128 rows (0 to 127, 128 to 255, ...) at most 64 rows name the same one
- route_weights: float32 [1024, 2], P('sp'), may hold values from 0.2 to 1.2
- gate_branch: bfloat16 [1024, 2048], P('sp', 'tp'), may hold values from -4 to 4
- states: float32 [1024, 2048], P('sp', 'tp'), may hold values from -6 to 6
- decay: float32 [1024, 2048], P('sp', 'tp'), may hold values from 0 to 1
- w_proj: bfloat16 [2048, 2048], P(None, 'tp'), may hold values from -0.125 to 0.125
- w_gate: bfloat16 [8, 2048, 2048], P('sp', 'tp'), may hold values from -0.125 to 0.125
- w_up: bfloat16 [8, 2048, 2048], P('sp', 'tp'), may hold values from -0.125 to 0.125
- w_down: bfloat16 [8, 2048, 2048], P('sp', 'tp'), may hold values from -0.125 to 0.125
Outputs:
- grad_w_gate: bfloat16 [8, 2048, 2048], P('sp', 'tp')
- grad_w_up: bfloat16 [8, 2048, 2048], P('sp', 'tp')
- grad_w_down: bfloat16 [8, 2048, 2048], P('sp', 'tp')
- grad_w_proj: float32 [2048, 2048], P('sp', 'tp')
- grad_branch: bfloat16 [1024, 2048], P('sp', 'tp')
- grad_drive: float32 [1024, 2048], P('sp', 'tp')
- grad_decay: float32 [1024, 2048], P('sp', 'tp')
The draws below stay inside these ranges and needn't reach their ends.
Inputs may be any that keep to these rules, and one draw needn't show every extreme that they name: `route_ids`: each row names 2 different experts. In the rows of one index of sp no expert is named more than 64 times, a bound that some block reaches.
All inputs are finite; a program needn't handle non-finite values.
Results may differ from the reference program's by a relative error of at most 0.02.
Values may be sent and summed in bfloat16 or wider, within the bound.
A program may use at most 64 MiB of HBM per device.

```python
import math
import jax
import jax.numpy as jnp
import numpy as np
from jax import lax

D = 2048
D_RNN = 2048
F = 2048
TOP = 2
TOK_DEV = 128
EXPERTS = 8
TOKENS = 1024
CAP = 64
N_SP = 8
N_TP = 4


def draw_decay(key, part):
    keys = jax.random.split(jax.random.fold_in(key, 17), 5)
    fast_share = 0.5
    fast = jax.random.uniform(keys[0], (D_RNN,), jnp.float32) < fast_share
    slow_rate = jax.random.uniform(keys[1], (D_RNN,), jnp.float32, 0.25, 0.8) / TOKENS
    fast_rate = jnp.exp(jax.random.uniform(keys[2], (D_RNN,), jnp.float32, jnp.log(0.01), jnp.log(1.0 / 30.0)))
    base_rate = jnp.where(fast, fast_rate, slow_rate)
    spans = TOKENS // 64
    factor = jnp.exp(jax.random.uniform(keys[3], (spans, 1), jnp.float32, jnp.log(0.4), jnp.log(1.6)))
    noise = jax.random.uniform(keys[4], (TOKENS, D_RNN), jnp.float32, 0.5, 1.5)
    return jnp.exp(-(base_rate[None, :] * jnp.repeat(factor, 64, axis=0) * noise))


def strengthened(array, own_key, source, target, shards_of, factor):
    owner, partner = [(jnp.arange(array.shape[dim]) // (array.shape[dim] // shards_of)).reshape([-1 if axis == dim else 1 for axis in range(array.ndim)]) for dim in (source, target)]
    chosen = jax.random.permutation(own_key, shards_of)[partner]
    strong = (owner == chosen) | (owner == (partner + shards_of // 2) % shards_of)
    return jnp.where(strong, factor * array, array)


def levels(stream_key, extent, cuts, smallest, largest):
    def one(axis_at, shards_of):
        steps = jax.random.uniform(jax.random.fold_in(jax.random.fold_in(stream_key, 6), axis_at), (shards_of,), jnp.float32, smallest / len(cuts), largest / len(cuts))
        return jnp.repeat(jnp.exp(steps), extent[axis_at] // shards_of).reshape((-1,) + (1,) * (len(extent) - axis_at - 1))

    loudness = one(*cuts[0])
    for cut in cuts[1:]:
        loudness = loudness * one(*cut)
    return loudness


def shared_out(key, own, number, rows, amount, top, most, skew):
    sequence = jax.random.permutation(key, amount)
    crowded, common = shares(amount, rows * top, most, skew, True), shares(amount, rows * top, most, skew, False)
    places = jnp.arange(amount)

    def named(lengths, turn):
        used = int((lengths > 0).sum())
        fixed = max(1, used // 4)
        passed = fixed + (places - fixed + turn * (used - fixed)) % max(1, amount - fixed)
        return jnp.zeros((amount,), jnp.int32).at[sequence[jnp.where(places < fixed, places, passed)]].set(jnp.asarray(lengths, jnp.int32))

    lengths = jnp.where(number % 4 == 0, named(crowded, number // 4), named(common, number - number // 4 - 1))
    mixed = jax.random.permutation(jax.random.fold_in(own, 3), amount)
    giver, receiver = mixed[0:amount // 2 * 2:2], mixed[1:amount // 2 * 2:2]
    margin = jnp.minimum(lengths[giver] - 1, most - lengths[receiver]) // 2
    margin = jnp.where((giver == sequence[0]) | (receiver == sequence[0]) | (lengths[receiver] == 0), 0, jnp.maximum(margin, 0))
    passed = jax.random.randint(jax.random.fold_in(own, 4), (amount // 2,), 0, 1 << 20) % (margin + 1)
    lengths = lengths.at[giver].add(-passed).at[receiver].add(passed)
    items = jnp.searchsorted(jnp.cumsum(lengths), jnp.arange(rows * top), side="right").astype(jnp.int32)
    listing = items.reshape(top, rows).T
    listing = listing[jax.random.permutation(jax.random.fold_in(own, 1), rows)]
    turn = jax.random.randint(jax.random.fold_in(own, 2), (rows, 1), 0, top)
    return jnp.take_along_axis(listing, (jnp.arange(top)[None, :] + turn) % top, axis=1)


def shares(count, total, limit, lean, full):
    weights = [(1 << 20) // math.isqrt(grade ** lean) + 1 for grade in range(1, count + 1)]
    largest = limit if full else min(limit, max(-(-total // count), total * weights[0] // sum(weights)))
    least = 1 if total - largest >= count - 1 else 0
    counts, rest = [largest] + [least] * (count - 1), total - largest - least * (count - 1)
    while rest > 0:
        movable = [i for i in range(1, count) if counts[i] < largest] or [i for i in range(1, count) if counts[i] < limit]
        mass, left = sum([weights[i] for i in movable]), rest
        for i in movable:
            extra = min(limit - counts[i], max(1, left * weights[i] // mass), rest)
            counts[i] = counts[i] + extra
            rest = rest - extra
    return np.array(counts)


def bell_draw(stream_key, dims, width, most, cuts=(), kind=jnp.bfloat16):
    entries = jax.random.normal(stream_key, dims, jnp.float32) * width
    if len(cuts) > 0:
        entries = levels(stream_key, dims, cuts, -0.22, 0.18) * entries
    return jnp.clip(entries, min=-most, max=most).astype(kind)


def noise_with(stream_key, shape, deviation, bound, shards, heavy, kind=jnp.bfloat16):
    entries = deviation * jax.random.normal(stream_key, shape, jnp.float32)
    if shards:
        entries = entries * levels(stream_key, shape, shards, -0.22, 0.18)
    return jnp.clip(strengthened(entries, jax.random.fold_in(stream_key, 3), *heavy), -bound, bound).astype(kind)


def setup_inputs(seed: int = 0) -> dict:
    key_list = jax.random.split(jax.random.key(seed), 12)
    mixer_out = bell_draw(key_list[0], (TOKENS, D), 1.0, 6.0, ((0, 8),))
    out_grad = noise_with(key_list[1], (TOKENS, D), 0.25, 2.0, ((0, 8),), (0, 1, 8, 2.0))
    route_ids_keys = jax.random.split(jax.random.fold_in(key_list[2], 1), TOKENS // TOK_DEV)
    route_ids_turns = jax.random.permutation(jax.random.fold_in(key_list[2], 3), TOKENS // TOK_DEV)
    route_ids = jax.vmap(lambda own, number: shared_out(jax.random.fold_in(key_list[2], 2), own, number, TOK_DEV, EXPERTS, TOP, CAP, 1))(route_ids_keys, route_ids_turns).reshape((TOKENS, TOP))
    route_weights = jnp.clip(0.2 + 1 * jax.random.uniform(key_list[3], (TOKENS, TOP), jnp.float32) ** levels(key_list[3], (TOKENS, TOP), ((0, 8),), -0.2, 0.2), 0.2, 1.2)
    gate_branch = bell_draw(key_list[4], (TOKENS, D_RNN), 0.5, 4.0, ((0, 8), (1, 4)))
    states = bell_draw(key_list[5], (TOKENS, D_RNN), 1.0, 6.0, ((0, 8), (1, 4)), jnp.float32)
    decay = draw_decay(jax.random.fold_in(key_list[11], 71), 0)
    w_proj = bell_draw(key_list[7], (D, D_RNN), D_RNN ** -0.5, 0.125, ((1, 4),))
    w_gate = bell_draw(key_list[8], (EXPERTS, F, D), D ** -0.5, 0.125, ((0, 8), (1, 4)))
    w_up = bell_draw(key_list[9], (EXPERTS, F, D), D ** -0.5, 0.125, ((0, 8), (1, 4)))
    w_down = bell_draw(key_list[10], (EXPERTS, F, D), F ** -0.5, 0.125, ((0, 8), (1, 4)))
    return dict(mixer_out=mixer_out, out_grad=out_grad, route_ids=route_ids, route_weights=route_weights, gate_branch=gate_branch, states=states, decay=decay, w_proj=w_proj, w_gate=w_gate, w_up=w_up, w_down=w_down)


def linear_combine(earlier, later):
    return earlier[0] * later[0], later[0] * earlier[1] + later[1]


def reference(mixer_out, out_grad, route_ids, route_weights, gate_branch, states, decay, w_proj, w_gate, w_up, w_down):
    routes = TOKENS * TOP
    flat_ids = route_ids.reshape(-1).astype(jnp.int32)
    onehot = (flat_ids[:, None] == jnp.arange(EXPERTS, dtype=jnp.int32)[None, :]).astype(jnp.int32)
    counted = jnp.cumsum(onehot.reshape(N_SP, TOK_DEV * TOP, EXPERTS), axis=1).reshape(routes, EXPERTS)
    position = (jnp.sum(counted * onehot, axis=1) - 1).astype(jnp.int32)
    block_id = (jnp.arange(routes, dtype=jnp.int32) // (TOK_DEV * TOP)).astype(jnp.int32)
    slot_index = ((flat_ids * N_SP + block_id) * CAP + position).astype(jnp.int32)
    table = jnp.full((EXPERTS * N_SP * CAP,), routes, jnp.int32).at[slot_index].set(jnp.arange(routes, dtype=jnp.int32))
    table = table.reshape(EXPERTS, N_SP * CAP)
    scaled = (route_weights[:, :, None].astype(jnp.float32) * out_grad[:, None, :].astype(jnp.float32)).astype(jnp.bfloat16)
    scaled_pad = jnp.concatenate([scaled.reshape(routes, D), jnp.zeros((1, D), jnp.bfloat16)], axis=0)
    token_pad = jnp.concatenate([mixer_out, jnp.zeros((1, D), jnp.bfloat16)], axis=0)

    def one_expert(carry, expert):
        slot_routes = table[expert]
        inputs = token_pad[slot_routes // TOP].astype(jnp.float32)
        cotangents = scaled_pad[slot_routes].astype(jnp.float32)
        weight_gate = w_gate[expert].astype(jnp.float32)
        weight_up = w_up[expert].astype(jnp.float32)
        weight_down = w_down[expert].astype(jnp.float32)
        gate_pre = jnp.dot(inputs, weight_gate.T, preferred_element_type=jnp.float32)
        up_pre = jnp.dot(inputs, weight_up.T, preferred_element_type=jnp.float32)
        sigmoid_gate = jax.nn.sigmoid(gate_pre)
        silu_gate = gate_pre * sigmoid_gate
        hidden = (silu_gate * up_pre).astype(jnp.bfloat16).astype(jnp.float32)
        hidden_grad = jnp.dot(cotangents, weight_down.T, preferred_element_type=jnp.float32)
        up_grad = (hidden_grad * silu_gate).astype(jnp.bfloat16).astype(jnp.float32)
        gate_grad = (hidden_grad * up_pre * sigmoid_gate * (1.0 + gate_pre * (1.0 - sigmoid_gate))).astype(jnp.bfloat16).astype(jnp.float32)
        grad_gate = jnp.dot(gate_grad.T, inputs, preferred_element_type=jnp.float32).astype(jnp.bfloat16)
        grad_up = jnp.dot(up_grad.T, inputs, preferred_element_type=jnp.float32).astype(jnp.bfloat16)
        grad_down = jnp.dot(hidden.T, cotangents, preferred_element_type=jnp.float32).astype(jnp.bfloat16)
        slots = slot_routes.shape[0]
        block_part = jnp.einsum("sbf,bfd->sbd", gate_grad.reshape(slots, N_TP, F // N_TP), weight_gate.reshape(N_TP, F // N_TP, D))
        block_part = block_part + jnp.einsum("sbf,bfd->sbd", up_grad.reshape(slots, N_TP, F // N_TP), weight_up.reshape(N_TP, F // N_TP, D))
        partial_value = jnp.sum(block_part.astype(jnp.bfloat16).astype(jnp.float32), axis=1)
        carry = carry.at[slot_routes].add(partial_value)
        return carry, (grad_gate, grad_up, grad_down)

    start_carry = jnp.zeros((routes + 1, D), jnp.float32)
    route_grad, stacked = lax.scan(one_expert, start_carry, jnp.arange(EXPERTS, dtype=jnp.int32))
    grad_w_gate, grad_w_up, grad_w_down = stacked
    routed_grad = jnp.sum(route_grad[:routes].reshape(TOKENS, TOP, D), axis=1)
    mid_grad = (out_grad.astype(jnp.float32) + routed_grad).astype(jnp.bfloat16)
    gated = (gate_branch.astype(jnp.float32) * states).astype(jnp.bfloat16)
    grad_w_proj = jnp.dot(mid_grad.T, gated, preferred_element_type=jnp.float32)
    act_grad = jnp.dot(mid_grad, w_proj, preferred_element_type=jnp.float32)
    grad_branch = (act_grad * states).astype(jnp.bfloat16)
    state_grad = act_grad * gate_branch.astype(jnp.float32)
    next_decay = jnp.concatenate([decay[1:], jnp.ones((1, D_RNN), jnp.float32)], axis=0)
    decay_prod, flipped = lax.associative_scan(linear_combine, (next_decay[::-1], state_grad[::-1]), axis=0)
    grad_drive = flipped[::-1]
    previous = jnp.concatenate([jnp.zeros((1, D_RNN), jnp.float32), states[:-1]], axis=0)
    grad_decay = grad_drive * previous
    return grad_w_gate, grad_w_up, grad_w_down, grad_w_proj, grad_branch, grad_drive, grad_decay
```

```python
import functools

import jax
import jax.numpy as jnp
from jax import lax
from jax.experimental import pallas as pl
from jax.experimental.pallas import tpu as pltpu
from jax.sharding import PartitionSpec as P

MESH = pl.DeviceIdType.MESH
F32 = jnp.float32
BF16 = jnp.bfloat16
CHUNKS = 2


def dot(a, b, ca, cb):
    return lax.dot_general(a, b, (((ca,), (cb,)), ((), ())), preferred_element_type=F32)


def kernel(
    n_sp,
    n_tp,
    ids,
    wts,
    mix,
    og,
    gb,
    st,
    dc,
    wp_h,
    wg_h,
    wu_h,
    wd_h,
    dwg_h,
    dwu_h,
    dwd_h,
    gproj,
    gbr,
    gdr,
    gdc,
    wp,
    wg,
    wu,
    wd,
    dwg,
    dwu,
    dwd,
    sel,
    send,
    xc,
    ga,
    pv,
    gg,
    ug,
    hid,
    pb,
    po,
    rc,
    qb,
    ry,
    fb,
    ret,
    mt,
    mr,
    cs,
    cr,
    w_sem,
    o_sem,
    l_sem,
    sp_s,
    sp_r,
    core_s,
    core_r,
    y_s,
    y_r,
    ga_s,
    ga_r,
    pv_sem,
    pc_s,
    pc_r,
    py_s,
    py_r,
    ret_s,
    ret_r,
    mt_s,
    mt_r,
    mr_s,
    mr_r,
    c_s,
    c_r,
):
    i = lax.axis_index("sp")
    t = lax.axis_index("tp")
    ny = n_tp // 2
    y, c = t // 2, t % 2
    tok = mix.shape[0]
    cap = xc.shape[3]
    dg = xc.shape[4]
    half = n_sp // CHUNKS
    rows = half * cap
    slots = n_sp * cap
    peer = (i, y * 2 + 1 - c)

    def columns(g):
        return pl.ds(pl.multiple_of(g * dg, dg), dg)

    def later(k):
        return lax.rem(i + k, n_sp)

    def before(k):
        return lax.rem(i + n_sp - k, n_sp)

    def y_up(q):
        return lax.rem(y + q, ny)

    def remote(src, dst, s, r, who):
        return pltpu.make_async_remote_copy(
            src_ref=src, dst_ref=dst, send_sem=s, recv_sem=r, device_id=who, device_id_type=MESH
        )

    loads = [
        pltpu.make_async_copy(a, b, w_sem.at[n])
        for n, (a, b) in enumerate(((wg_h, wg), (wu_h, wu), (wd_h, wd), (wp_h, wp)))
    ]
    for load in loads:
        load.start()

    barrier = pltpu.get_barrier_semaphore()
    for k in range(1, n_sp):
        pl.semaphore_signal(barrier, inc=1, device_id=(later(k), t), device_id_type=MESH)
    for k in range(1, n_tp):
        pl.semaphore_signal(
            barrier, inc=1, device_id=(i, lax.rem(t + k, n_tp)), device_id_type=MESH
        )

    experts_iota = lax.broadcasted_iota(jnp.int32, (n_sp, tok), 0)
    named = jnp.zeros((n_sp, tok), F32)
    weight = jnp.zeros((n_sp, tok), F32)
    for k in range(ids.shape[0]):
        hit = ids[k : k + 1, :] == experts_iota
        named = jnp.where(hit, 1.0, named)
        weight = jnp.where(hit, wts[k : k + 1, :], weight)
    earlier = (
        lax.broadcasted_iota(jnp.int32, (tok, tok), 0)
        < lax.broadcasted_iota(jnp.int32, (tok, tok), 1)
    )
    place = dot(named.astype(BF16), jnp.where(earlier, 1.0, 0.0).astype(BF16), 1, 0)
    place = jnp.where(named > 0.5, place, -1.0).astype(jnp.int32)
    slot_iota = lax.broadcasted_iota(jnp.int32, (cap, tok), 0)
    mix_part = mix[:, columns(t)]
    og_part = og[:, columns(t)]
    for e in range(n_sp):
        here = jnp.where(place[e : e + 1, :] == slot_iota, 1.0, 0.0)
        slot_weight = jnp.sum(here * weight[e : e + 1, :], axis=1, keepdims=True)
        here = here.astype(BF16)
        sel[e * cap : (e + 1) * cap, :] = here
        send[0, e] = dot(here, mix_part, 1, 0).astype(BF16)
        send[1, e] = (dot(here, og_part, 1, 0) * slot_weight).astype(BF16)

    ga[i] = (gb[...].astype(F32) * st[...]).astype(BF16)
    pl.semaphore_wait(barrier, n_sp + n_tp - 2)

    pending = []

    def go(copy):
        copy.start()
        pending.append(copy)

    own = pltpu.make_async_copy(send.at[:, i], xc.at[:, t, i], l_sem.at[0])
    own.start()

    def dispatch(k):
        return remote(
            send.at[:, later(k)], xc.at[:, t, i], sp_s.at[k], sp_r.at[k], (later(k), t)
        )

    for k in range(1, n_sp):
        go(dispatch(k))
    go(
        remote(
            st.at[pl.ds(tok - 8, 8)], pv, pv_sem.at[0], pv_sem.at[1], (later(1), t)
        )
    )
    pv_copy = pending[-1]

    def to_core(q, k):
        block = xc.at[:, 2 * y_up(q) + c, before(k)]
        return remote(block, block, core_s.at[q, k], core_r.at[q, k], peer)

    def to_y(q, k):
        block = xc.at[:, t, before(k)]
        return remote(
            block, block, y_s.at[q, k], y_r.at[q, k], (i, 2 * y_up(q) + c)
        )

    def from_y(q, k):
        block = xc.at[:, 2 * y_up(ny - q) + c, before(k)]
        return remote(block, block, y_s.at[q, k], y_r.at[q, k], (i, 2 * y_up(q) + c))

    def from_sp(k):
        return remote(
            send.at[:, later(k)], xc.at[:, t, before(k)], sp_s.at[k], sp_r.at[k], (later(k), t)
        )

    def from_core(q, k):
        block = xc.at[:, 2 * y_up(q) + 1 - c, before(k)]
        return remote(block, block, core_s.at[q, k], core_r.at[q, k], peer)

    def spread(k):
        if k == 0:
            own.wait()
        else:
            from_sp(k).wait_recv()
        for q in range(1, ny):
            go(to_y(q, k))
        go(to_core(0, k))

    def hand_on(k):
        for q in range(1, ny):
            from_y(q, k).wait_recv()
            go(to_core(ny - q, k))

    def expert(m):
        order = [before(m * half + q) for q in range(half)]

        def rows_of(which, g):
            return jnp.concatenate([xc[which, g, s] for s in order], axis=0)

        gate = up = hg = None
        for g in range(n_tp):
            cols = slice(g * dg, (g + 1) * dg)
            x, cot = rows_of(0, g), rows_of(1, g)
            parts = (dot(x, wg[:, cols], 1, 1), dot(x, wu[:, cols], 1, 1), dot(cot, wd[:, cols], 1, 1))
            if g == 0:
                gate, up, hg = parts
            else:
                gate, up, hg = gate + parts[0], up + parts[1], hg + parts[2]
        s = jax.nn.sigmoid(gate)
        silu = gate * s
        hidden = (silu * up).astype(BF16)
        up_grad = (hg * silu).astype(BF16)
        gate_grad = (hg * up * s * (1.0 + gate * (1.0 - s))).astype(BF16)
        for q, src in enumerate(order):
            part = slice(q * cap, (q + 1) * cap)
            hid[src] = hidden[part]
            ug[src] = up_grad[part]
            gg[src] = gate_grad[part]
        return gate_grad, up_grad

    def partial(gate_grad, up_grad, g):
        cols = columns(g)
        return (dot(gate_grad, wg[:, cols], 1, 0) + dot(up_grad, wu[:, cols], 1, 0)).astype(BF16)

    def swap_core(m, q):
        return remote(pb.at[m, q], rc.at[m, q], pc_s.at[m, q], pc_r.at[m, q], peer)

    def swap_y(m, q):
        return remote(
            qb.at[m, q], ry.at[m, q], py_s.at[m, q], py_r.at[m, q], (i, 2 * y_up(q) + c)
        )

    def partials(m, grads):
        for q in list(range(1, ny)) + [0]:
            pb[m, q] = partial(*grads, 2 * y_up(q) + 1 - c)
            go(swap_core(m, q))
        for q in list(range(1, ny)) + [0]:
            po[m, q] = partial(*grads, 2 * y_up(q) + c)

    def fold_core(m):
        for q in range(1, ny):
            swap_core(m, q).wait_recv()
            qb[m, q] = (po[m, q].astype(F32) + rc[m, q].astype(F32)).astype(BF16)
            go(swap_y(m, q))

    def home(k):
        m, q = k // half, k % half
        return remote(
            fb.at[m, pl.ds(q * cap, cap)], ret.at[i], ret_s.at[k], ret_r.at[k], (before(k), t)
        )

    def fold_y(m):
        swap_core(m, 0).wait_recv()
        total = po[m, 0].astype(F32) + rc[m, 0].astype(F32)
        for q in range(1, ny):
            swap_y(m, q).wait_recv()
            total = total + ry[m, q].astype(F32)
        fb[m] = total.astype(BF16)
        for q in range(half):
            k = m * half + q
            if k == 0:
                pltpu.make_async_copy(
                    fb.at[0, pl.ds(0, cap)], ret.at[i], l_sem.at[1]
                ).start()
            else:
                go(home(k))

    def weight_grad(left, which, out, out_h, n):
        a = left[...].reshape(slots, left.shape[2])
        for g in range(n_tp):
            b = xc[which, g].reshape(slots, dg)
            out[:, g * dg : (g + 1) * dg] = dot(a, b, 0, 0).astype(BF16)
        copy = pltpu.make_async_copy(out, out_h, o_sem.at[n])
        copy.start()
        return copy

    for k in range(n_sp):
        spread(k)
        if k >= 1:
            hand_on(k - 1)
    hand_on(n_sp - 1)

    def share_gated(k):
        return remote(ga.at[i], ga.at[i], ga_s.at[k], ga_r.at[k], (later(k), t))

    for k in range(1, n_sp):
        go(share_gated(k))
    for load in loads:
        load.wait()

    def arrived(m):
        for k in range(m * half, (m + 1) * half):
            for q in range(ny):
                from_core(q, k).wait_recv()

    arrived(0)
    grads = expert(0)
    partials(0, grads)
    arrived(1)
    grads = expert(1)
    fold_core(0)
    partials(1, grads)
    outs = [weight_grad(gg, 0, dwg, dwg_h, 0)]
    fold_core(1)
    fold_y(0)
    outs.append(weight_grad(ug, 0, dwu, dwu_h, 1))
    fold_y(1)
    outs.append(weight_grad(hid, 1, dwd, dwd_h, 2))

    pltpu.make_async_copy(fb.at[0, pl.ds(0, cap)], ret.at[i], l_sem.at[1]).wait()

    def from_expert(k):
        m, q = k // half, k % half
        return remote(
            fb.at[m, pl.ds(q * cap, cap)],
            ret.at[later(k)],
            ret_s.at[k],
            ret_r.at[k],
            (before(k), t),
        )

    for k in range(1, n_sp):
        from_expert(k).wait_recv()
    routed = dot(ret[...].reshape(slots, dg), sel[...], 0, 0)
    mid = (og[:, columns(t)].astype(F32).T + routed).astype(BF16)
    mt[t] = mid

    def share_mid(k):
        return remote(mt.at[t], mt.at[t], mt_s.at[k], mt_r.at[k], (i, lax.rem(t + k, n_tp)))

    def get_mid(k):
        block = mt.at[lax.rem(t + n_tp - k, n_tp)]
        return remote(block, block, mt_s.at[k], mt_r.at[k], (i, lax.rem(t + k, n_tp)))

    for k in range(1, n_tp):
        go(share_mid(k))

    row = lax.broadcasted_iota(jnp.int32, dc.shape, 0)
    decay = dc[...]
    head = decay[0:1, :]
    factor = jnp.where(row < tok - 1, pltpu.roll(decay, tok - 1, 0), 1.0)
    for k in range(1, n_tp):
        get_mid(k).wait_recv()

    share = mr.shape[1]
    per = dg // share if dg >= share else 1

    def rows_for(s):
        return mt.at[s // per, pl.ds(pl.multiple_of((s % per) * share, share), share)]

    def share_rows(k):
        return remote(rows_for(later(k)), mr.at[i], mr_s.at[k], mr_r.at[k], (later(k), t))

    def get_rows(k):
        return remote(rows_for(later(k)), mr.at[before(k)], mr_s.at[k], mr_r.at[k], (later(k), t))

    for k in range(1, n_sp):
        go(share_rows(k))
    own_rows = pltpu.make_async_copy(rows_for(i), mr.at[i], l_sem.at[2])
    own_rows.start()

    act = dot(mt[...].reshape(n_tp * dg, tok), wp[...], 0, 0)
    grad = act * gb[...].astype(F32)
    gbr[...] = (act * st[...]).astype(BF16)
    step = 1
    while step < tok:
        inside = row < tok - step
        grad = grad + jnp.where(inside, factor * pltpu.roll(grad, tok - step, 0), 0.0)
        factor = factor * jnp.where(inside, pltpu.roll(factor, tok - step, 0), 1.0)
        step *= 2
    pair = jnp.concatenate([head * factor[0:1, :], head * grad[0:1, :]], axis=0)
    pair = jnp.concatenate([pair, jnp.zeros((6, pair.shape[1]), F32)], axis=0)
    cs[...] = pair
    cr[i] = pair

    def share_carry(k):
        return remote(cs, cr.at[i], c_s.at[k], c_r.at[k], (later(k), t))

    def get_carry(k):
        return remote(cs, cr.at[before(k)], c_s.at[k], c_r.at[k], (later(k), t))

    for k in range(1, n_sp):
        go(share_carry(k))

    own_rows.wait()
    for k in range(1, n_sp):
        remote(ga.at[i], ga.at[before(k)], ga_s.at[k], ga_r.at[k], (later(k), t)).wait_recv()
    total = None
    for k in range(n_sp):
        if k:
            get_rows(k).wait_recv()
        src = before(k)
        term = dot(mr[src], ga[src], 1, 0)
        total = term if total is None else total + term
    gproj[...] = total

    for k in range(1, n_sp):
        get_carry(k).wait_recv()
    carry = jnp.zeros((1, pair.shape[1]), F32)
    for s in range(n_sp - 1, 0, -1):
        carry = jnp.where(s > i, cr[s, 1:2, :] + cr[s, 0:1, :] * carry, carry)
    drive = grad + factor * carry
    gdr[...] = drive
    pv_copy.wait_recv()
    states = st[...]
    last = jnp.where(i > 0, pv[7:8, :], 0.0)
    previous = jnp.where(row == 0, last, pltpu.roll(states, 1, 0))
    gdc[...] = drive * previous

    for copy in outs:
        copy.wait()
    for copy in pending:
        copy.wait_send()


def local(
    mixer_out,
    out_grad,
    route_ids,
    route_weights,
    gate_branch,
    states,
    decay,
    w_proj,
    w_gate,
    w_up,
    w_down,
):
    tok, width = mixer_out.shape
    top = route_ids.shape[1]
    n_sp, n_tp = lax.axis_size("sp"), lax.axis_size("tp")
    ny = n_tp // 2
    assert w_gate.shape[0] == 1
    cap = 2 * top * tok // n_sp
    dg = width // n_tp
    hidden = w_gate.shape[1]
    channels = states.shape[1]
    half_rows = n_sp * cap // CHUNKS
    share = width // n_sp
    vmem = pl.BlockSpec(memory_space=pltpu.VMEM)
    hbm = pl.BlockSpec(memory_space=pl.ANY)
    dma = pltpu.SemaphoreType.DMA
    weight = (hidden, width)
    outs = pl.pallas_call(
        functools.partial(kernel, n_sp, n_tp),
        out_shape=[jax.ShapeDtypeStruct(weight, BF16)] * 3
        + [
            jax.ShapeDtypeStruct((share, channels), F32),
            jax.ShapeDtypeStruct((tok, channels), BF16),
            jax.ShapeDtypeStruct((tok, channels), F32),
            jax.ShapeDtypeStruct((tok, channels), F32),
        ],
        in_specs=[vmem] * 7 + [hbm] * 4,
        out_specs=[hbm] * 3 + [vmem] * 4,
        scratch_shapes=[
            pltpu.VMEM((width, channels), BF16),
            *([pltpu.VMEM(weight, BF16)] * 6),
            pltpu.VMEM((n_sp * cap, tok), BF16),
            pltpu.VMEM((2, n_sp, cap, dg), BF16),
            pltpu.VMEM((2, n_tp, n_sp, cap, dg), BF16),
            pltpu.VMEM((n_sp, tok, channels), BF16),
            pltpu.VMEM((8, channels), F32),
            *([pltpu.VMEM((n_sp, cap, hidden), BF16)] * 3),
            *([pltpu.VMEM((CHUNKS, ny, half_rows, dg), BF16)] * 5),
            pltpu.VMEM((CHUNKS, half_rows, dg), BF16),
            pltpu.VMEM((n_sp, cap, dg), BF16),
            pltpu.VMEM((n_tp, dg, tok), BF16),
            pltpu.VMEM((n_sp, share, tok), BF16),
            pltpu.VMEM((8, channels), F32),
            pltpu.VMEM((n_sp, 8, channels), F32),
            dma((4,)),
            dma((3,)),
            dma((3,)),
            dma((n_sp,)),
            dma((n_sp,)),
            *([dma((ny, n_sp))] * 4),
            dma((n_sp,)),
            dma((n_sp,)),
            dma((2,)),
            *([dma((CHUNKS, ny))] * 4),
            dma((n_sp,)),
            dma((n_sp,)),
            dma((n_tp,)),
            dma((n_tp,)),
            *([dma((n_sp,))] * 4),
        ],
        compiler_params=pltpu.CompilerParams(
            collective_id=0, has_side_effects=True, vmem_limit_bytes=60 * 1024 * 1024
        ),
    )(
        route_ids.T,
        route_weights.T,
        mixer_out,
        out_grad,
        gate_branch,
        states,
        decay,
        w_proj,
        w_gate[0],
        w_up[0],
        w_down[0],
    )
    return (outs[0][None], outs[1][None], outs[2][None], *outs[3:])


def solution(mesh):
    placed = (
        P("sp", None),
        P("sp", None),
        P("sp", None),
        P("sp", None),
        P("sp", "tp"),
        P("sp", "tp"),
        P("sp", "tp"),
        P(None, "tp"),
        P("sp", "tp", None),
        P("sp", "tp", None),
        P("sp", "tp", None),
    )
    return jax.shard_map(
        local,
        mesh=mesh,
        in_specs=placed,
        out_specs=(
            P("sp", "tp", None),
            P("sp", "tp", None),
            P("sp", "tp", None),
            P("sp", "tp"),
            P("sp", "tp"),
            P("sp", "tp"),
            P("sp", "tp"),
        ),
        check_vma=False,
    )
```

```python
import functools

import jax
import jax.numpy as jnp
from jax import lax
from jax.experimental import pallas as pl
from jax.experimental.pallas import tpu as pltpu
from jax.sharding import PartitionSpec as P

MESH = pl.DeviceIdType.MESH
F32 = jnp.float32
BF16 = jnp.bfloat16
CHUNKS = 2


def dot(a, b, ca, cb):
    return lax.dot_general(a, b, (((ca,), (cb,)), ((), ())), preferred_element_type=F32)


def kernel(
    n_sp,
    n_tp,
    ids,
    wts,
    mix,
    og,
    gb,
    st,
    dc,
    wp_h,
    wg_h,
    wu_h,
    wd_h,
    dwg_h,
    dwu_h,
    dwd_h,
    gproj,
    gbr,
    gdr,
    gdc,
    wp,
    wg,
    wu,
    wd,
    dwg,
    dwu,
    dwd,
    sel,
    sw,
    send,
    xc,
    ga,
    pv,
    gg,
    ug,
    hid,
    pb,
    po,
    rc,
    qb,
    ry,
    fb,
    ret,
    mt,
    mr,
    cs,
    cr,
    w_sem,
    o_sem,
    l_sem,
    sp_s,
    sp_r,
    core_s,
    core_r,
    y_s,
    y_r,
    ga_s,
    ga_r,
    pv_sem,
    pc_s,
    pc_r,
    py_s,
    py_r,
    ret_s,
    ret_r,
    mtc_s,
    mtc_r,
    mty_s,
    mty_r,
    mr_s,
    mr_r,
    mrc_s,
    mrc_r,
    c_s,
    c_r,
):
    i = lax.axis_index("sp")
    t = lax.axis_index("tp")
    ny = n_tp // 2
    y, c = t // 2, t % 2
    tok = mix.shape[0]
    cap = xc.shape[3]
    dg = xc.shape[4]
    half = n_sp // CHUNKS
    rows = half * cap
    slots = n_sp * cap
    peer = (i, y * 2 + 1 - c)
    straight = ()

    def columns(g):
        return pl.ds(pl.multiple_of(g * dg, dg), dg)

    def later(k):
        return lax.rem(i + k, n_sp)

    def before(k):
        return lax.rem(i + n_sp - k, n_sp)

    def y_up(q):
        return lax.rem(y + q, ny)

    def remote(src, dst, s, r, who):
        return pltpu.make_async_remote_copy(
            src_ref=src, dst_ref=dst, send_sem=s, recv_sem=r, device_id=who, device_id_type=MESH
        )

    loads = [
        pltpu.make_async_copy(a, b, w_sem.at[n])
        for n, (a, b) in enumerate(((wg_h, wg), (wu_h, wu), (wd_h, wd), (wp_h, wp)))
    ]
    for load in loads:
        load.start()

    barrier = pltpu.get_barrier_semaphore()
    for k in range(1, n_sp):
        pl.semaphore_signal(barrier, inc=1, device_id=(later(k), t), device_id_type=MESH)
    for k in range(1, n_tp):
        pl.semaphore_signal(
            barrier, inc=1, device_id=(i, lax.rem(t + k, n_tp)), device_id_type=MESH
        )

    experts_iota = lax.broadcasted_iota(jnp.int32, (n_sp, tok), 0)
    named = jnp.zeros((n_sp, tok), F32)
    weight = jnp.zeros((n_sp, tok), F32)
    for k in range(ids.shape[0]):
        hit = ids[k : k + 1, :] == experts_iota
        named = jnp.where(hit, 1.0, named)
        weight = jnp.where(hit, wts[k : k + 1, :], weight)
    earlier = (
        lax.broadcasted_iota(jnp.int32, (tok, tok), 0)
        < lax.broadcasted_iota(jnp.int32, (tok, tok), 1)
    )
    place = dot(named.astype(BF16), jnp.where(earlier, 1.0, 0.0).astype(BF16), 1, 0)
    place = jnp.where(named > 0.5, place, -1.0).astype(jnp.int32)
    slot_iota = lax.broadcasted_iota(jnp.int32, (cap, tok), 0)
    for e in range(n_sp):
        here = jnp.where(place[e : e + 1, :] == slot_iota, 1.0, 0.0)
        slot_weight = jnp.sum(here * weight[e : e + 1, :], axis=1, keepdims=True)
        sel[e * cap : (e + 1) * cap, :] = here.astype(BF16)
        sw[e * cap : (e + 1) * cap, :] = jnp.broadcast_to(slot_weight, (cap, sw.shape[1]))
    chosen = sel[...]
    for q in range(ny):
        cols = columns(2 * y_up(q) + c)
        send[0, q] = dot(chosen, mix[:, cols], 1, 0).astype(BF16).reshape(n_sp, cap, dg)
        send[1, q] = (
            (dot(chosen, og[:, cols], 1, 0) * sw[:, 0:1]).astype(BF16).reshape(n_sp, cap, dg)
        )
    pl.semaphore_wait(barrier, n_sp + n_tp - 2)

    pending = []

    def go(copy):
        copy.start()
        pending.append(copy)

    def groups(k):
        return range(ny) if k in straight else range(1)

    def dispatch(q, k):
        return remote(
            send.at[:, q, later(k)],
            xc.at[:, 2 * y_up(q) + c, i],
            sp_s.at[q, k],
            sp_r.at[q, k],
            (later(k), t),
        )

    for k in range(1, n_sp):
        for q in groups(k):
            go(dispatch(q, k))
    go(
        remote(
            st.at[pl.ds(tok - 8, 8)], pv, pv_sem.at[0], pv_sem.at[1], (later(1), t)
        )
    )
    pv_copy = pending[-1]

    mine = pl.ds(pl.multiple_of(i * cap, cap), cap)
    here, slot_weight = sel[mine, :], sw[mine, 0:1]
    for g in range(n_tp):
        cols = slice(g * dg, (g + 1) * dg)
        xc[0, g, i] = dot(here, mix[:, cols], 1, 0).astype(BF16)
        xc[1, g, i] = (dot(here, og[:, cols], 1, 0) * slot_weight).astype(BF16)
    ga[i] = (gb[...].astype(F32) * st[...]).astype(BF16)

    def to_core(q, k):
        block = xc.at[:, 2 * y_up(q) + c, before(k)]
        return remote(block, block, core_s.at[q, k], core_r.at[q, k], peer)

    def to_y(q, k):
        block = xc.at[:, t, before(k)]
        return remote(
            block, block, y_s.at[q, k], y_r.at[q, k], (i, 2 * y_up(q) + c)
        )

    def from_y(q, k):
        block = xc.at[:, 2 * y_up(ny - q) + c, before(k)]
        return remote(block, block, y_s.at[q, k], y_r.at[q, k], (i, 2 * y_up(q) + c))

    def from_sp(q, k):
        return remote(
            send.at[:, q, later(k)],
            xc.at[:, 2 * y_up(q) + c, before(k)],
            sp_s.at[q, k],
            sp_r.at[q, k],
            (later(k), t),
        )

    def from_core(q, k):
        block = xc.at[:, 2 * y_up(q) + 1 - c, before(k)]
        return remote(block, block, core_s.at[q, k], core_r.at[q, k], peer)

    def spread(k):
        for q in groups(k):
            from_sp(q, k).wait_recv()
        if k not in straight:
            for q in range(1, ny):
                go(to_y(q, k))
        for q in groups(k):
            go(to_core(q, k))

    def hand_on(k):
        if k in straight:
            return
        for q in range(1, ny):
            from_y(q, k).wait_recv()
            go(to_core(ny - q, k))

    def expert(m):
        order = [before(m * half + q) for q in range(half)]

        def rows_of(which, g):
            return jnp.concatenate([xc[which, g, s] for s in order], axis=0)

        gate = up = hg = None
        for g in range(n_tp):
            cols = slice(g * dg, (g + 1) * dg)
            x, cot = rows_of(0, g), rows_of(1, g)
            parts = (dot(x, wg[:, cols], 1, 1), dot(x, wu[:, cols], 1, 1), dot(cot, wd[:, cols], 1, 1))
            if g == 0:
                gate, up, hg = parts
            else:
                gate, up, hg = gate + parts[0], up + parts[1], hg + parts[2]
        s = jax.nn.sigmoid(gate)
        silu = gate * s
        hidden = (silu * up).astype(BF16)
        up_grad = (hg * silu).astype(BF16)
        gate_grad = (hg * up * s * (1.0 + gate * (1.0 - s))).astype(BF16)
        for q, src in enumerate(order):
            part = slice(q * cap, (q + 1) * cap)
            hid[src] = hidden[part]
            ug[src] = up_grad[part]
            gg[src] = gate_grad[part]
        return gate_grad, up_grad

    def partial(gate_grad, up_grad, g):
        cols = columns(g)
        return (dot(gate_grad, wg[:, cols], 1, 0) + dot(up_grad, wu[:, cols], 1, 0)).astype(BF16)

    def swap_core(m, q):
        return remote(pb.at[m, q], rc.at[m, q], pc_s.at[m, q], pc_r.at[m, q], peer)

    def swap_y(m, q):
        return remote(
            qb.at[m, q], ry.at[m, q], py_s.at[m, q], py_r.at[m, q], (i, 2 * y_up(q) + c)
        )

    def partials(m, grads):
        for q in list(range(1, ny)) + [0]:
            pb[m, q] = partial(*grads, 2 * y_up(q) + 1 - c)
            go(swap_core(m, q))
        for q in list(range(1, ny)) + [0]:
            po[m, q] = partial(*grads, 2 * y_up(q) + c)

    def fold_core(m):
        for q in range(1, ny):
            swap_core(m, q).wait_recv()
            qb[m, q] = (po[m, q].astype(F32) + rc[m, q].astype(F32)).astype(BF16)
            go(swap_y(m, q))

    def home(k):
        m, q = k // half, k % half
        return remote(
            fb.at[m, pl.ds(q * cap, cap)], ret.at[i], ret_s.at[k], ret_r.at[k], (before(k), t)
        )

    def fold_y(m):
        swap_core(m, 0).wait_recv()
        total = po[m, 0].astype(F32) + rc[m, 0].astype(F32)
        for q in range(1, ny):
            swap_y(m, q).wait_recv()
            total = total + ry[m, q].astype(F32)
        fb[m] = total.astype(BF16)
        for q in range(half):
            k = m * half + q
            if k == 0:
                pltpu.make_async_copy(
                    fb.at[0, pl.ds(0, cap)], ret.at[i], l_sem.at[1]
                ).start()
            else:
                go(home(k))

    def weight_grad(left, which, out, out_h, n):
        a = left[...].reshape(slots, left.shape[2])
        for g in range(n_tp):
            b = xc[which, g].reshape(slots, dg)
            out[:, g * dg : (g + 1) * dg] = dot(a, b, 0, 0).astype(BF16)
        copy = pltpu.make_async_copy(out, out_h, o_sem.at[n])
        copy.start()
        return copy

    for k in range(1, n_sp):
        spread(k)
        if 1 < k <= half:
            hand_on(k - 1)

    pair_peer = (i + 1 - 2 * (i % 2), t)

    def share_gated(k):
        return remote(ga.at[i], ga.at[i], ga_s.at[k], ga_r.at[k], (later(k), t))

    def get_gated(k):
        return remote(ga.at[i], ga.at[before(k)], ga_s.at[k], ga_r.at[k], (later(k), t))

    def pass_gated(k):
        block = ga.at[before(k)]
        return remote(block, block, ga_s.at[k + 1], ga_r.at[k + 1], pair_peer)

    def passed_gated(k):
        block = ga.at[lax.rem(pair_peer[0] + n_sp - k, n_sp)]
        return remote(block, block, ga_s.at[k + 1], ga_r.at[k + 1], pair_peer)

    for k in range(2, n_sp, 2):
        go(share_gated(k))
    for load in loads:
        load.wait()

    def arrived(m):
        for k in range(max(1, m * half), (m + 1) * half):
            for q in range(ny):
                from_core(q, k).wait_recv()

    arrived(0)
    grads = expert(0)
    for k in range(half, n_sp):
        hand_on(k)
    partials(0, grads)
    arrived(1)
    grads = expert(1)
    fold_core(0)
    partials(1, grads)
    outs = [weight_grad(gg, 0, dwg, dwg_h, 0)]
    fold_core(1)
    fold_y(0)
    outs.append(weight_grad(ug, 0, dwu, dwu_h, 1))
    fold_y(1)
    outs.append(weight_grad(hid, 1, dwd, dwd_h, 2))
    for k in range(0, n_sp, 2):
        if k:
            get_gated(k).wait_recv()
        go(pass_gated(k))

    pltpu.make_async_copy(fb.at[0, pl.ds(0, cap)], ret.at[i], l_sem.at[1]).wait()

    def from_expert(k):
        m, q = k // half, k % half
        return remote(
            fb.at[m, pl.ds(q * cap, cap)],
            ret.at[later(k)],
            ret_s.at[k],
            ret_r.at[k],
            (before(k), t),
        )

    for k in range(1, n_sp):
        from_expert(k).wait_recv()
    routed = dot(ret[...].reshape(slots, dg), sel[...], 0, 0)
    mid = (og[:, columns(t)].astype(F32).T + routed).astype(BF16)
    mt[t] = mid

    def mid_core(q):
        block = mt.at[2 * y_up(q) + c]
        return remote(block, block, mtc_s.at[q], mtc_r.at[q], peer)

    def mid_from_core(q):
        block = mt.at[2 * y_up(q) + 1 - c]
        return remote(block, block, mtc_s.at[q], mtc_r.at[q], peer)

    def mid_y(q):
        return remote(mt.at[t], mt.at[t], mty_s.at[q], mty_r.at[q], (i, 2 * y_up(q) + c))

    def mid_from_y(q):
        block = mt.at[2 * y_up(ny - q) + c]
        return remote(block, block, mty_s.at[q], mty_r.at[q], (i, 2 * y_up(q) + c))

    for q in range(1, ny):
        go(mid_y(q))
    go(mid_core(0))

    row = lax.broadcasted_iota(jnp.int32, dc.shape, 0)
    decay = dc[...]
    head = decay[0:1, :]
    factor = jnp.where(row < tok - 1, pltpu.roll(decay, tok - 1, 0), 1.0)
    for q in range(1, ny):
        mid_from_y(q).wait_recv()
        go(mid_core(ny - q))
    for q in range(ny):
        mid_from_core(q).wait_recv()

    share = 2 * mr.shape[2]
    per = dg // share if dg >= share else 1

    part = share // 2

    def rows_for(s, h):
        first = (s % per) * share + h * part
        return mt.at[s // per, pl.ds(pl.multiple_of(first, part), part)]

    def share_rows(k):
        return remote(rows_for(later(k), c), mr.at[i, c], mr_s.at[k], mr_r.at[k], (later(k), t))

    def get_rows(k):
        return remote(
            rows_for(later(k), c), mr.at[before(k), c], mr_s.at[k], mr_r.at[k], (later(k), t)
        )

    def swap_rows(k, h):
        block = mr.at[before(k), h]
        return remote(block, block, mrc_s.at[k], mrc_r.at[k], peer)

    for k in range(1, n_sp):
        go(share_rows(k))
    for h in range(2):
        own_rows = pltpu.make_async_copy(rows_for(i, h), mr.at[i, h], l_sem.at[h])
        own_rows.start()
        own_rows.wait()

    act = dot(mt[...].reshape(n_tp * dg, tok), wp[...], 0, 0)
    grad = act * gb[...].astype(F32)
    gbr[...] = (act * st[...]).astype(BF16)
    step = 1
    while step < tok:
        inside = row < tok - step
        grad = grad + jnp.where(inside, factor * pltpu.roll(grad, tok - step, 0), 0.0)
        factor = factor * jnp.where(inside, pltpu.roll(factor, tok - step, 0), 1.0)
        step *= 2
    pair = jnp.concatenate([head * factor[0:1, :], head * grad[0:1, :]], axis=0)
    pair = jnp.concatenate([pair, jnp.zeros((6, pair.shape[1]), F32)], axis=0)
    cs[...] = pair
    cr[i] = pair

    def share_carry(k):
        return remote(cs, cr.at[i], c_s.at[k], c_r.at[k], (later(k), t))

    def get_carry(k):
        return remote(cs, cr.at[before(k)], c_s.at[k], c_r.at[k], (later(k), t))

    for k in range(1, n_sp):
        go(share_carry(k))

    for k in range(1, n_sp):
        get_rows(k).wait_recv()
        go(swap_rows(k, c))
    for k in range(0, n_sp, 2):
        passed_gated(k).wait_recv()
    total = None
    for k in range(n_sp):
        if k:
            swap_rows(k, 1 - c).wait_recv()
        src = before(k)
        term = dot(mr[src].reshape(share, tok), ga[src], 1, 0)
        total = term if total is None else total + term
    gproj[...] = total

    for k in range(1, n_sp):
        get_carry(k).wait_recv()
    carry = jnp.zeros((1, pair.shape[1]), F32)
    for s in range(n_sp - 1, 0, -1):
        carry = jnp.where(s > i, cr[s, 1:2, :] + cr[s, 0:1, :] * carry, carry)
    drive = grad + factor * carry
    gdr[...] = drive
    pv_copy.wait_recv()
    states = st[...]
    last = jnp.where(i > 0, pv[7:8, :], 0.0)
    previous = jnp.where(row == 0, last, pltpu.roll(states, 1, 0))
    gdc[...] = drive * previous

    for copy in outs:
        copy.wait()
    for copy in pending:
        copy.wait_send()


def settle(count, *refs):
    ins, outs, held = refs[:count], refs[count : 2 * count], refs[2 * count : 3 * count]
    in_sem, out_sem = refs[3 * count :]
    jobs = []
    for n in range(count):
        pieces = 2 if n < 3 else 1
        rows = ins[n].shape[0] // pieces
        for p in range(pieces):
            part = pl.ds(p * rows, rows)
            jobs.append(
                (
                    pltpu.make_async_copy(ins[n].at[part], held[n].at[part], in_sem.at[n, p]),
                    pltpu.make_async_copy(held[n].at[part], outs[n].at[part], out_sem.at[n, p]),
                )
            )
    for bring, _ in jobs:
        bring.start()
    for bring, put in jobs:
        bring.wait()
        put.start()
    for _, put in jobs:
        put.wait()


def local(
    mixer_out,
    out_grad,
    route_ids,
    route_weights,
    gate_branch,
    states,
    decay,
    w_proj,
    w_gate,
    w_up,
    w_down,
):
    tok, width = mixer_out.shape
    top = route_ids.shape[1]
    n_sp, n_tp = lax.axis_size("sp"), lax.axis_size("tp")
    ny = n_tp // 2
    assert w_gate.shape[0] == 1
    cap = 2 * top * tok // n_sp
    dg = width // n_tp
    hidden = w_gate.shape[1]
    channels = states.shape[1]
    half_rows = n_sp * cap // CHUNKS
    share = width // n_sp
    vmem = pl.BlockSpec(memory_space=pltpu.VMEM)
    hbm = pl.BlockSpec(memory_space=pl.ANY)
    dma = pltpu.SemaphoreType.DMA
    weight = (hidden, width)
    outs = pl.pallas_call(
        functools.partial(kernel, n_sp, n_tp),
        out_shape=[jax.ShapeDtypeStruct(weight, BF16)] * 3
        + [
            jax.ShapeDtypeStruct((share, channels), F32),
            jax.ShapeDtypeStruct((tok, channels), BF16),
            jax.ShapeDtypeStruct((tok, channels), F32),
            jax.ShapeDtypeStruct((tok, channels), F32),
        ],
        in_specs=[vmem] * 7 + [hbm] * 4,
        out_specs=[hbm] * 3 + [vmem] * 4,
        scratch_shapes=[
            pltpu.VMEM((width, channels), BF16),
            *([pltpu.VMEM(weight, BF16)] * 6),
            pltpu.VMEM((n_sp * cap, tok), BF16),
            pltpu.VMEM((n_sp * cap, 128), F32),
            pltpu.VMEM((2, ny, n_sp, cap, dg), BF16),
            pltpu.VMEM((2, n_tp, n_sp, cap, dg), BF16),
            pltpu.VMEM((n_sp, tok, channels), BF16),
            pltpu.VMEM((8, channels), F32),
            *([pltpu.VMEM((n_sp, cap, hidden), BF16)] * 3),
            *([pltpu.VMEM((CHUNKS, ny, half_rows, dg), BF16)] * 5),
            pltpu.VMEM((CHUNKS, half_rows, dg), BF16),
            pltpu.VMEM((n_sp, cap, dg), BF16),
            pltpu.VMEM((n_tp, dg, tok), BF16),
            pltpu.VMEM((n_sp, 2, share // 2, tok), BF16),
            pltpu.VMEM((8, channels), F32),
            pltpu.VMEM((n_sp, 8, channels), F32),
            dma((4,)),
            dma((3,)),
            dma((3,)),
            *([dma((ny, n_sp))] * 6),
            dma((n_sp,)),
            dma((n_sp,)),
            dma((2,)),
            *([dma((CHUNKS, ny))] * 4),
            dma((n_sp,)),
            dma((n_sp,)),
            *([dma((ny,))] * 4),
            *([dma((n_sp,))] * 6),
        ],
        compiler_params=pltpu.CompilerParams(
            collective_id=0, has_side_effects=True, vmem_limit_bytes=60 * 1024 * 1024
        ),
    )(
        route_ids.T,
        route_weights.T,
        mixer_out,
        out_grad,
        gate_branch,
        states,
        decay,
        w_proj,
        w_gate[0],
        w_up[0],
        w_down[0],
    )
    count = len(outs)
    outs = pl.pallas_call(
        functools.partial(settle, count),
        out_shape=[jax.ShapeDtypeStruct(o.shape, o.dtype) for o in outs],
        in_specs=[hbm] * count,
        out_specs=[hbm] * count,
        scratch_shapes=[
            *(pltpu.VMEM(o.shape, o.dtype) for o in outs),
            dma((count, 2)),
            dma((count, 2)),
        ],
    )(*outs)
    return (outs[0][None], outs[1][None], outs[2][None], *outs[3:])


def solution(mesh):
    placed = (
        P("sp", None),
        P("sp", None),
        P("sp", None),
        P("sp", None),
        P("sp", "tp"),
        P("sp", "tp"),
        P("sp", "tp"),
        P(None, "tp"),
        P("sp", "tp", None),
        P("sp", "tp", None),
        P("sp", "tp", None),
    )
    return jax.shard_map(
        local,
        mesh=mesh,
        in_specs=placed,
        out_specs=(
            P("sp", "tp", None),
            P("sp", "tp", None),
            P("sp", "tp", None),
            P("sp", "tp"),
            P("sp", "tp"),
            P("sp", "tp"),
            P("sp", "tp"),
        ),
        check_vma=False,
    )
```
